32 devices in a mesh: grp: 2 (over y), fs: 4 (over z), tp: 4 (over x, core).
Axes of the slice: x: 2, y: 2, z: 4, core: 2. Of those that a mesh axis runs over, the one named last changes fastest.
Arguments:
- tokens: bfloat16 [4096, 2048], P(('grp', 'fs')), parts along dimension 0, may hold values from -6 to 6
- norm_gain: float32 [2, 2048], replicated, may hold values from 0.1 to 1.9
- norm_shift: float32 [2, 2048], replicated, may hold values from -3 to 3
- gate_first: bfloat16 [2048, 3072], P('fs', 'tp'), may hold values from -0.125 to 0.125
- up_first: bfloat16 [2048, 3072], P('fs', 'tp'), may hold values from -0.125 to 0.125
- down_first: bfloat16 [3072, 2048], P('tp', 'fs'), may hold values from -0.21875 to 0.21875
- gate_second: bfloat16 [2048, 3072], P('fs', 'tp'), may hold values from -0.125 to 0.125
- up_second: bfloat16 [2048, 3072], P('fs', 'tp'), may hold values from -0.125 to 0.125
- down_second: bfloat16 [3072, 2048], P('tp', 'fs'), may hold values from -0.21875 to 0.21875
Outputs:
- encoded: bfloat16 [4096, 2048], P(('grp', 'fs')), parts along dimension 0
The draws below stay inside these ranges and needn't reach their ends.
There are 2 independent parts, one for each index of `grp`. The reference program is written for one: setup_inputs(seed, part) draws one part's arguments, and reference() takes and returns one part's arrays. A program takes and returns all parts, laid end to end along the dimension named above; an argument that names none is the same for every part. Nothing has to cross between parts.
All inputs are finite; a program needn't handle non-finite values.
Results may differ from the reference program's by a relative error of at most 0.012.
Values may be sent and summed in bfloat16 or wider, within the bound.
A program may use at most 64 MiB of HBM per device.

```python
import jax
import jax.numpy as jnp
from jax import lax

D = 2048
FF = 3072
TOKENS = 2048
N_TP = 4


def block_scale(rng, extent, cuts, smallest, largest):
    def one(dim, blocks):
        steps = jax.random.uniform(jax.random.fold_in(jax.random.fold_in(rng, 6), dim), (blocks,), jnp.float32, smallest / len(cuts), largest / len(cuts))
        return jnp.repeat(jnp.exp(steps), extent[dim] // blocks).reshape((-1,) + (1,) * (len(extent) - dim - 1))

    factor_of = one(*cuts[0])
    for cut in cuts[1:]:
        factor_of = factor_of * one(*cut)
    return factor_of


def bell_draw(own_key, shape, scale, reach, cuts=(), kind=jnp.bfloat16):
    result = jax.random.normal(own_key, shape, jnp.float32) * scale
    if len(cuts) > 0:
        result = block_scale(own_key, shape, cuts, -0.22, 0.18) * result
    return jnp.clip(result, min=-reach, max=reach).astype(kind)


def setup_inputs(seed: int = 0, part: int = 0) -> dict:
    arg_keys = jax.random.split(jax.random.key(seed), 10)
    part_splits = jax.random.split(jax.random.fold_in(arg_keys[9], part), 10)
    tokens = bell_draw(part_splits[0], (TOKENS, D), 1.0, 6.0, ((0, 4),))
    norm_gain = jnp.clip(1.0 + 0.18 * jax.random.normal(arg_keys[1], (2, D), jnp.float32), 0.1, 1.9)
    norm_shift = bell_draw(arg_keys[2], (2, D), 0.5, 3.0, (), jnp.float32)
    gate_first = bell_draw(arg_keys[3], (D, FF), D ** -0.5, 0.125, ((0, 4), (1, 4)))
    up_first = bell_draw(arg_keys[4], (D, FF), D ** -0.5, 0.125, ((0, 4), (1, 4)))
    down_first = bell_draw(arg_keys[5], (FF, D), (FF // 4) ** -0.5, 0.21875, ((0, 4), (1, 4)))
    gate_second = bell_draw(arg_keys[6], (D, FF), D ** -0.5, 0.125, ((0, 4), (1, 4)))
    up_second = bell_draw(arg_keys[7], (D, FF), D ** -0.5, 0.125, ((0, 4), (1, 4)))
    down_second = bell_draw(arg_keys[8], (FF, D), (FF // 4) ** -0.5, 0.21875, ((0, 4), (1, 4)))
    return {"tokens": tokens, "norm_gain": norm_gain, "norm_shift": norm_shift, "gate_first": gate_first, "up_first": up_first, "down_first": down_first, "gate_second": gate_second, "up_second": up_second, "down_second": down_second}


def post_norm(values, gain, shift):
    mean = lax.optimization_barrier(jnp.mean(values, axis=-1, keepdims=True))
    spread = lax.optimization_barrier(jnp.mean(jnp.square(values - mean), axis=-1, keepdims=True))
    normed = (values - mean) * lax.rsqrt(spread + 1e-05)
    return (normed * gain + shift).astype(jnp.bfloat16)

def feed_forward(stream, gate_w, up_w, down_w):
    gate = jnp.dot(stream, gate_w, preferred_element_type=jnp.float32)
    up = jnp.dot(stream, up_w, preferred_element_type=jnp.float32)
    hidden = (jax.nn.silu(gate) * up).astype(jnp.bfloat16)
    width = FF // N_TP
    total = jnp.zeros((stream.shape[0], down_w.shape[1]), jnp.float32)
    for block in range(N_TP):
        partial_value = jnp.dot(hidden[:, block * width:(block + 1) * width], down_w[block * width:(block + 1) * width], preferred_element_type=jnp.float32).astype(jnp.bfloat16)
        partial_value = lax.optimization_barrier(partial_value)
        total = total + partial_value.astype(jnp.float32)
    return total.astype(jnp.bfloat16)

def reference(tokens, norm_gain, norm_shift, gate_first, up_first, down_first, gate_second, up_second, down_second):
    scale = 2.0 ** 0.25
    branch = feed_forward(tokens, gate_first, up_first, down_first)
    middle = post_norm(scale * tokens.astype(jnp.float32) + 0.5 * branch.astype(jnp.float32), norm_gain[0], norm_shift[0])
    branch2 = feed_forward(middle, gate_second, up_second, down_second)
    return post_norm(scale * middle.astype(jnp.float32) + 0.5 * branch2.astype(jnp.float32), norm_gain[1], norm_shift[1])
```

```python
import functools

import jax
import jax.numpy as jnp
from jax import lax
from jax.experimental import pallas as pl
from jax.experimental.pallas import tpu as pltpu
from jax.sharding import PartitionSpec as P

MESH = pl.DeviceIdType.MESH
SCALE = 2.0**0.25
F32 = jnp.float32
BF16 = jnp.bfloat16


def aligned(value, step):
    return pl.multiple_of(value, step)


def fused_kernel(nf, nt, *refs):
    tokens, gains, shifts = refs[:3]
    shards = refs[3:9]
    out = refs[9]
    full = refs[10:16]
    gate, hidden, part, middle, pair, ring = refs[16:22]
    z_recv, y_recv, right_sent, left_sent, y_sent, own_done = refs[22:28]
    core_sent, core_recv, x_sent, x_recv, swap_sent, swap_recv = refs[28:34]

    g = lax.axis_index("grp")
    f = lax.axis_index("fs")
    t = lax.axis_index("tp")
    other_g = 1 - g
    chip, core = t // 2, t % 2
    chips = nt // 2
    peer = chip * 2 + (1 - core)
    rows, width = tokens.shape
    half = rows // 2
    depth = width // nf

    def tell(**where):
        pl.semaphore_signal(barrier, inc=1, device_id=where, device_id_type=MESH)

    barrier = pltpu.get_barrier_semaphore()
    pl.when(f > 0)(lambda: tell(fs=f - 1))
    pl.when(f < nf - 1)(lambda: tell(fs=f + 1))
    tell(grp=other_g)
    tell(tp=peer)
    for step in range(1, chips):
        tell(tp=lax.rem(chip + step, chips) * 2 + core)
    ends = jnp.where(f > 0, 1, 0) + jnp.where(f < nf - 1, 1, 0)
    pl.semaphore_wait(barrier, ends + 1 + chips)

    def shard_part(a, which):
        size = shards[a].shape[0] // 2
        return shards[a].at[pl.ds(aligned(which * size, size), size), :]

    def slot(a, s, which):
        if a % 3 == 2:
            size = full[a].shape[1] // 2
            return full[a].at[s, pl.ds(aligned(which * size, size), size), :]
        size = depth // 2
        return full[a].at[pl.ds(aligned(s * depth + which * size, size), size), :]

    def whole_slot(a, s):
        if a % 3 == 2:
            return full[a].at[s]
        return full[a].at[pl.ds(aligned(s * depth, depth), depth), :]

    def own(a):
        return pltpu.make_async_copy(shards[a], whole_slot(a, f), own_done.at[a])

    def to_right(a, s, src):
        return pltpu.make_async_remote_copy(
            src, slot(a, s, g), right_sent.at[a, s], z_recv.at[a, s],
            device_id={"fs": f + 1}, device_id_type=MESH)

    def to_left(a, s, src):
        return pltpu.make_async_remote_copy(
            src, slot(a, s, g), left_sent.at[a, s], z_recv.at[a, s],
            device_id={"fs": f - 1}, device_id_type=MESH)

    def across(a, s, which):
        return pltpu.make_async_remote_copy(
            slot(a, s, which), slot(a, s, which), y_sent.at[a, s], y_recv.at[a, s],
            device_id={"grp": other_g}, device_id_type=MESH)

    def send_own(a):
        pl.when(f < nf - 1)(lambda: to_right(a, f, shard_part(a, g)).start())
        pl.when(f > 0)(lambda: to_left(a, f, shard_part(a, g)).start())

    def hop(a, h):
        @pl.when(f - h >= 0)
        def _():
            s = f - h
            to_left(a, s, slot(a, s, g)).wait_recv()
            pl.when(f < nf - 1)(lambda: to_right(a, s, slot(a, s, g)).start())
            across(a, s, g).start()

        @pl.when(f + h < nf)
        def _():
            s = f + h
            to_right(a, s, slot(a, s, g)).wait_recv()
            pl.when(f > 0)(lambda: to_left(a, s, slot(a, s, g)).start())
            across(a, s, g).start()

    def at_distance(h, work):
        if h == 0:
            work(f)
            return
        pl.when(f - h >= 0)(lambda: work(f - h))
        pl.when(f + h < nf)(lambda: work(f + h))

    def crossed(a, s):
        across(a, s, other_g).wait_recv()

    def arrived(a):
        own(a).wait()
        for h in range(1, nf):
            at_distance(h, lambda s: crossed(a, s))

    tile = 256 if gate.shape[1] % 256 == 0 else gate.shape[1]

    def project_gate(a, stream):
        @pl.loop(0, gate.shape[1] // tile)
        def _(i):
            cols = pl.ds(aligned(i * tile, tile), tile)
            gate[:, cols] = jnp.dot(stream[...], full[a][:, cols], preferred_element_type=F32)

    def project_up(a, stream):
        @pl.loop(0, gate.shape[1] // tile)
        def _(i):
            cols = pl.ds(aligned(i * tile, tile), tile)
            up = jnp.dot(stream[...], full[a][:, cols], preferred_element_type=F32)
            hidden[:, cols] = (jax.nn.silu(gate[:, cols]) * up).astype(BF16)

    def columns(s):
        return pl.ds(aligned(s * depth, depth), depth)

    mine = pl.ds(aligned(core * half, half), half)
    theirs = pl.ds(aligned((1 - core) * half, half), half)

    def core_copy(layer, s):
        return pltpu.make_async_remote_copy(
            part.at[layer, theirs, columns(s)], pair.at[layer, :, columns(s)],
            core_sent.at[layer, s], core_recv.at[layer, s],
            device_id={"tp": peer}, device_id_type=MESH)

    def x_copy(layer, s, source, target):
        return pltpu.make_async_remote_copy(
            ring.at[layer, source, :, columns(s)], ring.at[layer, source, :, columns(s)],
            x_sent.at[layer, s, target], x_recv.at[layer, s, source],
            device_id={"tp": target * 2 + core}, device_id_type=MESH)

    def partial(layer, s):
        part[layer, :, columns(s)] = jnp.dot(
            hidden[...], full[3 * layer + 2][s], preferred_element_type=F32).astype(BF16)
        core_copy(layer, s).start()

    def pair_sum(layer, s):
        core_copy(layer, s).wait_recv()
        ring[layer, chip, :, columns(s)] = (
            part[layer, mine, columns(s)].astype(F32) + pair[layer, :, columns(s)].astype(F32)
        ).astype(BF16)
        for step in range(1, chips):
            x_copy(layer, s, chip, lax.rem(chip + step, chips)).start()

    def chips_in(layer, s):
        for step in range(1, chips):
            source = lax.rem(chip + step, chips)
            x_copy(layer, s, source, source).wait_recv()

    def swap_copy(layer, target):
        return pltpu.make_async_remote_copy(
            target.at[mine, :], target.at[mine, :], swap_sent.at[layer], swap_recv.at[layer],
            device_id={"tp": peer}, device_id_type=MESH)

    def swap_in(layer, target):
        return pltpu.make_async_remote_copy(
            target.at[theirs, :], target.at[theirs, :], swap_sent.at[layer], swap_recv.at[layer],
            device_id={"tp": peer}, device_id_type=MESH)

    def norm(layer, stream, target):
        band = 32

        @pl.loop(0, half // band)
        def _(i):
            here = pl.ds(aligned(i * band, band), band)
            there = pl.ds(aligned(core * half + i * band, band), band)
            total = ring[layer, 0, here, :].astype(F32)
            for c in range(1, chips):
                total = total + ring[layer, c, here, :].astype(F32)
            branch = total.astype(BF16).astype(F32)
            v = SCALE * stream[there, :].astype(F32) + 0.5 * branch
            mean = jnp.mean(v, axis=-1, keepdims=True)
            v = v - mean
            spread = jnp.mean(v * v, axis=-1, keepdims=True)
            normed = v * lax.rsqrt(spread + 1e-05)
            target[there, :] = (
                normed * gains[layer:layer + 1, :] + shifts[layer:layer + 1, :]).astype(BF16)

        swap_copy(layer, target).start()
        swap_in(layer, target).wait_recv()

    def all_shards(work):
        for h in range(nf):
            at_distance(h, work)

    for a in range(2):
        send_own(a)
    for a in range(6):
        own(a).start()

    for a in range(5):
        if a > 0:
            send_own(a + 1)
        hop(a, 1)
        if a == 1:
            arrived(0)
            project_gate(0, tokens)
        if a == 2:
            arrived(1)
            project_up(1, tokens)
        if a == 3:
            arrived(2)

            @pl.loop(0, nf)
            def _(s):
                partial(0, s)

            @pl.loop(0, nf)
            def _(s):
                pair_sum(0, s)

        if a == 4:
            @pl.loop(0, nf)
            def _(s):
                chips_in(0, s)

            norm(0, tokens, middle)
            arrived(3)
            project_gate(3, middle)
        for h in range(2, nf):
            hop(a, h)

    hop(5, 1)
    arrived(4)
    project_up(4, middle)
    own(5).wait()
    partial(1, f)
    for h in range(2, nf + 1):
        if h < nf:
            hop(5, h)

        def finish(s):
            crossed(5, s)
            partial(1, s)

        at_distance(h - 2, lambda s: pair_sum(1, s))
        at_distance(h - 1, finish)
    at_distance(nf - 1, lambda s: pair_sum(1, s))

    @pl.loop(0, nf)
    def _(s):
        chips_in(1, s)

    norm(1, middle, out)

    for a in range(6):
        @pl.loop(0, nf)
        def _(s):
            pl.when((s <= f) & (f < nf - 1))(lambda: to_right(a, s, slot(a, s, g)).wait_send())
            pl.when((s >= f) & (f > 0))(lambda: to_left(a, s, slot(a, s, g)).wait_send())
            pl.when(s != f)(lambda: across(a, s, g).wait_send())

    for layer in range(2):
        @pl.loop(0, nf)
        def _(s):
            core_copy(layer, s).wait_send()
            for step in range(1, chips):
                x_copy(layer, s, chip, lax.rem(chip + step, chips)).wait_send()

    swap_copy(0, middle).wait_send()
    swap_copy(1, out).wait_send()


def fused(nf, nt, tokens, gains, shifts, *weights):
    rows, width = tokens.shape
    units = weights[0].shape[1]
    depth = width // nf
    side = pltpu.VMEM((width, units), BF16)
    down = pltpu.VMEM((nf, units, depth), BF16)
    dma = pltpu.SemaphoreType.DMA
    chips = nt // 2
    return pl.pallas_call(
        functools.partial(fused_kernel, nf, nt),
        out_shape=jax.ShapeDtypeStruct((rows, width), BF16),
        in_specs=[pl.BlockSpec(memory_space=pltpu.VMEM)] * 3
        + [pl.BlockSpec(memory_space=pl.ANY)] * 6,
        out_specs=pl.BlockSpec(memory_space=pltpu.VMEM),
        scratch_shapes=[
            side, side, down, side, side, down,
            pltpu.VMEM((rows, units), F32),
            pltpu.VMEM((rows, units), BF16),
            pltpu.VMEM((2, rows, width), BF16),
            pltpu.VMEM((rows, width), BF16),
            pltpu.VMEM((2, rows // 2, width), BF16),
            pltpu.VMEM((2, chips, rows // 2, width), BF16),
            dma((6, nf)), dma((6, nf)), dma((6, nf)), dma((6, nf)), dma((6, nf)), dma((6,)),
            dma((2, nf)), dma((2, nf)), dma((2, nf, chips)), dma((2, nf, chips)),
            dma((2,)), dma((2,)),
        ],
        compiler_params=pltpu.CompilerParams(
            collective_id=0, has_side_effects=True, vmem_limit_bytes=60 * 1024 * 1024),
    )(tokens, gains, shifts, *weights)


def post_norm(values, gain, shift):
    mean = jnp.mean(values, axis=-1, keepdims=True)
    spread = jnp.mean(jnp.square(values - mean), axis=-1, keepdims=True)
    normed = (values - mean) * lax.rsqrt(spread + 1e-05)
    return (normed * gain + shift).astype(jnp.bfloat16)


def rounded_term(stream_rows, down_full):
    return jnp.dot(stream_rows, down_full, preferred_element_type=jnp.float32).astype(jnp.bfloat16)


def half_step(stream, gate_w, up_w, down_w, gain, shift):
    width = gate_w.shape[1]
    joined = jnp.concatenate(
        (
            lax.all_gather(gate_w, "fs", axis=0, tiled=True),
            lax.all_gather(up_w, "fs", axis=0, tiled=True),
        ),
        axis=1,
    )
    both = jnp.dot(stream, joined, preferred_element_type=jnp.float32)
    gate = both[:, :width]
    up = both[:, width:]
    hidden = (jax.nn.silu(gate) * up).astype(jnp.bfloat16)
    scale = 2.0**0.25
    down_full = lax.all_gather(down_w, "fs", axis=1, tiled=True)
    partial_value = rounded_term(hidden, down_full)
    branch = lax.psum(partial_value, "tp").astype(jnp.float32).astype(jnp.bfloat16)
    return post_norm(
        scale * stream.astype(jnp.float32) + 0.5 * branch.astype(jnp.float32), gain, shift
    )


def local(
    tokens,
    norm_gain,
    norm_shift,
    gate_first,
    up_first,
    down_first,
    gate_second,
    up_second,
    down_second,
):
    middle = half_step(tokens, gate_first, up_first, down_first, norm_gain[0], norm_shift[0])
    return half_step(middle, gate_second, up_second, down_second, norm_gain[1], norm_shift[1])


def fits(mesh, args):
    tokens, gate_first = args[0], args[3]
    nf, nt = mesh.shape["fs"], mesh.shape["tp"]
    depth, units = gate_first.shape
    return (
        mesh.shape["grp"] == 2 and nt % 2 == 0 and 1 < nf <= 8
        and depth % 128 == 0 and units % 128 == 0 and tokens.shape[0] % 64 == 0
    )


def solution(mesh):
    def either(*args):
        if fits(mesh, args):
            return fused(mesh.shape["fs"], mesh.shape["tp"], *args)
        return local(*args)

    placed = (
        P(("grp", "fs"), None),
        P(),
        P(),
        P("fs", "tp"),
        P("fs", "tp"),
        P("tp", "fs"),
        P("fs", "tp"),
        P("fs", "tp"),
        P("tp", "fs"),
    )
    return jax.shard_map(
        either, mesh=mesh, in_specs=placed, out_specs=P(("grp", "fs"), None), check_vma=False
    )
```

```python
import functools

import jax
import jax.numpy as jnp
from jax import lax
from jax.experimental import pallas as pl
from jax.experimental.pallas import tpu as pltpu
from jax.sharding import PartitionSpec as P

MESH = pl.DeviceIdType.MESH
SCALE = 2.0**0.25
F32 = jnp.float32
BF16 = jnp.bfloat16


def aligned(value, step):
    return pl.multiple_of(value, step)


def fused_kernel(nf, nt, *refs):
    gains, shifts, tokens = refs[:3]
    shards = refs[3:9]
    out = refs[9]
    full = refs[10:16]
    stream, gate, hidden, part, middle, pair, ring = refs[16:23]
    (z_recv, extra_recv, y_recv, line_sent, mate_sent, extra_sent, y_sent, own_done,
     core_sent, core_recv, x_sent, x_recv, back_sent, back_recv,
     swap_sent, swap_recv, hand_sent, hand_recv, tokens_done) = refs[23:]

    g = lax.axis_index("grp")
    f = lax.axis_index("fs")
    t = lax.axis_index("tp")
    other_g = 1 - g
    chip, core = t // 2, t % 2
    chips = nt // 2
    peer = chip * 2 + (1 - core)
    rows, width = tokens.shape
    half = rows // 2
    depth = width // nf

    at_end = (f == 0) | (f == nf - 1)
    inside = (f > 0) & (f < nf - 1)
    low = f < nf // 2
    mate = jnp.where(low, 1 - f, 2 * nf - 3 - f)
    facing = nf - 1 - f
    far = nf - 1 - mate
    mine = pl.ds(aligned(core * half, half), half)
    theirs = pl.ds(aligned((1 - core) * half, half), half)

    def tell(**where):
        pl.semaphore_signal(barrier, inc=1, device_id=where, device_id_type=MESH)

    barrier = pltpu.get_barrier_semaphore()
    tell(fs=mate)
    pl.when(inside)(lambda: tell(fs=facing))
    tell(grp=other_g)
    tell(tp=peer)
    for step in range(1, chips):
        tell(tp=lax.rem(chip + step, chips) * 2 + core)
    pl.semaphore_wait(barrier, jnp.where(inside, 1, 0) + 2 + chips)

    def remote(src, dst, sent, received, **where):
        return pltpu.make_async_remote_copy(
            src, dst, sent, received, device_id=where, device_id_type=MESH)

    def shard_part(a, which):
        size = shards[a].shape[0] // 2
        return shards[a].at[pl.ds(aligned(which * size, size), size), :]

    def slot(a, s, which):
        if a % 3 == 2:
            size = full[a].shape[1] // 2
            return full[a].at[s, pl.ds(aligned(which * size, size), size), :]
        size = depth // 2
        return full[a].at[pl.ds(aligned(s * depth + which * size, size), size), :]

    def whole_slot(a, s):
        if a % 3 == 2:
            return full[a].at[s]
        return full[a].at[pl.ds(aligned(s * depth, depth), depth), :]

    def columns(s):
        return pl.ds(aligned(s * depth, depth), depth)

    both_parts = range(1, 6)

    def own(a):
        return pltpu.make_async_copy(shards[a], whole_slot(a, f), own_done.at[a])

    def from_end(a, s):
        return remote(shard_part(a, g), slot(a, s, g), mate_sent.at[a], z_recv.at[a, s], fs=mate)

    def extra(a, s):
        return remote(
            shard_part(a, other_g), slot(a, s, other_g), extra_sent.at[a], extra_recv.at[a],
            fs=mate)

    def along(a, s, src):
        return remote(src, slot(a, s, g), line_sent.at[a, s], z_recv.at[a, s], fs=facing)

    def across(a, s, which):
        return remote(
            slot(a, s, which), slot(a, s, which), y_sent.at[a, s], y_recv.at[a, s], grp=other_g)

    def hand_tokens():
        return remote(
            tokens.at[mine, :], stream.at[1, mine, :], hand_sent.at[0], hand_recv.at[0], fs=mate)

    def share_tokens(where):
        return remote(
            stream.at[1, where, :], stream.at[1, where, :], hand_sent.at[1], hand_recv.at[1],
            tp=peer)

    def hand_middle():
        return remote(
            middle.at[1, mine, :], middle.at[0, mine, :], hand_sent.at[2], hand_recv.at[2],
            fs=mate)

    def core_copy(layer, s):
        return remote(
            part.at[layer, :, theirs, columns(s)], pair.at[layer, :, :, columns(s)],
            core_sent.at[layer, s], core_recv.at[layer, s], tp=peer)

    def x_view(layer, s, source):
        if layer == 0:
            return ring.at[0, source, :, :, columns(s)]
        return ring.at[1, source, 0, :, columns(s)]

    def x_copy(layer, s, source, target):
        return remote(
            x_view(layer, s, source), x_view(layer, s, source),
            x_sent.at[layer, s, target], x_recv.at[layer, s, source], tp=target * 2 + core)

    def back(s):
        return remote(
            ring.at[1, chip, 1, :, columns(s)], ring.at[1, chip, 0, :, columns(s)],
            back_sent.at[s], back_recv.at[s], fs=mate)

    def swap(layer, where):
        view = middle.at[:, where, :] if layer == 0 else out.at[where, :]
        return remote(view, view, swap_sent.at[layer], swap_recv.at[layer], tp=peer)

    def x_start(layer, s):
        for step in range(1, chips):
            x_copy(layer, s, chip, lax.rem(chip + step, chips)).start()

    def x_arrived(layer, s):
        for step in range(1, chips):
            source = lax.rem(chip + step, chips)
            x_copy(layer, s, source, source).wait_recv()

    def x_left(layer, s):
        for step in range(1, chips):
            x_copy(layer, s, chip, lax.rem(chip + step, chips)).wait_send()

    tile = 256 if gate.shape[2] % 256 == 0 else gate.shape[2]
    tiles = gate.shape[2] // tile

    def project_gate(a, source):
        @pl.loop(0, 2 * tiles)
        def _(i):
            block, cols = i // tiles, pl.ds(aligned((i % tiles) * tile, tile), tile)
            gate[block, :, cols] = jnp.dot(
                source[block], full[a][:, cols], preferred_element_type=F32)

    def project_up(a, source):
        @pl.loop(0, 2 * tiles)
        def _(i):
            block, cols = i // tiles, pl.ds(aligned((i % tiles) * tile, tile), tile)
            up = jnp.dot(source[block], full[a][:, cols], preferred_element_type=F32)
            hidden[block, :, cols] = (jax.nn.silu(gate[block, :, cols]) * up).astype(BF16)

    def partial(layer, s):
        @pl.loop(0, 2)
        def _(block):
            part[layer, block, :, columns(s)] = jnp.dot(
                hidden[block], full[3 * layer + 2][s], preferred_element_type=F32).astype(BF16)
        core_copy(layer, s).start()

    def pair_sum(layer, s):
        core_copy(layer, s).wait_recv()
        for block in (1, 0):
            ring[layer, chip, block, :, columns(s)] = (
                part[layer, block, mine, columns(s)].astype(F32)
                + pair[layer, block, :, columns(s)].astype(F32)
            ).astype(BF16)
            if layer == 1 and block == 1:
                back(s).start()
        x_start(layer, s)

    def norm(layer, block, source, target):
        band = 32

        @pl.loop(0, half // band)
        def _(i):
            here = pl.ds(aligned(i * band, band), band)
            there = pl.ds(aligned(core * half + i * band, band), band)
            total = ring[layer, 0, block, here, :].astype(F32)
            for c in range(1, chips):
                total = total + ring[layer, c, block, here, :].astype(F32)
            branch = total.astype(BF16).astype(F32)
            v = SCALE * source[block, there, :].astype(F32) + 0.5 * branch
            v = v - jnp.mean(v, axis=-1, keepdims=True)
            spread = jnp.mean(v * v, axis=-1, keepdims=True)
            normed = v * lax.rsqrt(spread + 1e-05)
            done = (normed * gains[layer:layer + 1, :] + shifts[layer:layer + 1, :]).astype(BF16)
            if layer == 0:
                target[block, there, :] = done
            else:
                target[there, :] = done

    def finish():
        norm(1, 0, middle, out)
        swap(1, mine).start()
        swap(1, theirs).wait_recv()
        swap(1, mine).wait_send()

    @pl.when(at_end)
    def _():
        from_end(0, f).start()
        hand_tokens().start()
        for a in range(1, 6):
            from_end(a, f).start()
            if a in both_parts:
                extra(a, f).start()
        hand_middle().wait_recv()
        for s in (mate, f, nf - 1 - mate, nf - 1 - f):
            back(s).wait_recv()
            x_start(1, s)
        pl.loop(0, nf)(lambda s: x_arrived(1, s))
        finish()
        hand_tokens().wait_send()
        for a in range(6):
            from_end(a, f).wait_send()
            if a in both_parts:
                extra(a, f).wait_send()
        pl.loop(0, nf)(lambda s: x_left(1, s))

    def mate_part(a):
        from_end(a, mate).wait_recv()
        along(a, mate, slot(a, mate, g)).start()
        if a not in both_parts:
            across(a, mate, g).start()

    def line_part(a, s):
        along(a, s, slot(a, s, g)).wait_recv()
        across(a, s, g).start()

    def mate_whole(a):
        if a in both_parts:
            extra(a, mate).wait_recv()
        else:
            across(a, mate, other_g).wait_recv()

    def crossed(a, s):
        across(a, s, other_g).wait_recv()

    def arrived(a):
        own(a).wait()
        mate_whole(a)
        crossed(a, facing)
        crossed(a, far)

    @pl.when(inside)
    def _():
        along(0, f, shard_part(0, g)).start()
        own_tokens = pltpu.make_async_copy(tokens, stream.at[0], tokens_done)
        own_tokens.start()
        for a in range(6):
            own(a).start()

        for a in range(6):
            if a < 5:
                along(a + 1, f, shard_part(a + 1, g)).start()
            if a == 0:
                line_part(a, facing)
                mate_part(a)
            else:
                mate_part(a)
                line_part(a, facing)
            if a == 1:
                hand_tokens().wait_recv()
                share_tokens(mine).start()
                own_tokens.wait()
                share_tokens(theirs).wait_recv()
                arrived(0)
                project_gate(0, stream)
            if a == 2:
                arrived(1)
                project_up(1, stream)
            if a == 3:
                arrived(2)
                pl.loop(0, nf)(lambda s: partial(0, s))
                pl.loop(0, nf)(lambda s: pair_sum(0, s))
            line_part(a, far)

        pl.loop(0, nf)(lambda s: x_arrived(0, s))
        norm(0, 0, stream, middle)
        norm(0, 1, stream, middle)
        swap(0, mine).start()
        hand_middle().start()
        swap(0, theirs).wait_recv()
        arrived(3)
        project_gate(3, middle)
        arrived(4)
        project_up(4, middle)
        own(5).wait()
        partial(1, f)
        mate_whole(5)
        partial(1, mate)
        pair_sum(1, f)
        crossed(5, facing)
        partial(1, facing)
        pair_sum(1, mate)
        crossed(5, far)
        partial(1, far)
        pair_sum(1, facing)
        pair_sum(1, far)
        pl.loop(0, nf)(lambda s: x_arrived(1, s))
        finish()

        share_tokens(mine).wait_send()
        hand_middle().wait_send()
        swap(0, mine).wait_send()
        for a in range(6):
            along(a, f, slot(a, f, g)).wait_send()
            along(a, mate, slot(a, mate, g)).wait_send()
            across(a, facing, g).wait_send()
            across(a, far, g).wait_send()
            if a not in both_parts:
                across(a, mate, g).wait_send()

        @pl.loop(0, nf)
        def _(s):
            back(s).wait_send()
            for layer in range(2):
                core_copy(layer, s).wait_send()
                x_left(layer, s)


def fused(nf, nt, tokens, gains, shifts, *weights):
    rows, width = tokens.shape
    units = weights[0].shape[1]
    depth = width // nf
    half = rows // 2
    side = pltpu.VMEM((width, units), BF16)
    down = pltpu.VMEM((nf, units, depth), BF16)
    dma = pltpu.SemaphoreType.DMA
    chips = nt // 2
    return pl.pallas_call(
        functools.partial(fused_kernel, nf, nt),
        out_shape=jax.ShapeDtypeStruct((rows, width), BF16),
        in_specs=[pl.BlockSpec(memory_space=pltpu.VMEM)] * 2
        + [pl.BlockSpec(memory_space=pl.ANY)] * 7,
        out_specs=pl.BlockSpec(memory_space=pltpu.VMEM),
        scratch_shapes=[
            side, side, down, side, side, down,
            pltpu.VMEM((2, rows, width), BF16),
            pltpu.VMEM((2, rows, units), F32),
            pltpu.VMEM((2, rows, units), BF16),
            pltpu.VMEM((2, 2, rows, width), BF16),
            pltpu.VMEM((2, rows, width), BF16),
            pltpu.VMEM((2, 2, half, width), BF16),
            pltpu.VMEM((2, chips, 2, half, width), BF16),
            dma((6, nf)), dma((6,)), dma((6, nf)), dma((6, nf)), dma((6,)), dma((6,)),
            dma((6, nf)), dma((6,)),
            dma((2, nf)), dma((2, nf)), dma((2, nf, chips)), dma((2, nf, chips)),
            dma((nf,)), dma((nf,)),
            dma((2,)), dma((2,)), dma((3,)), dma((3,)), dma,
        ],
        compiler_params=pltpu.CompilerParams(
            collective_id=0, has_side_effects=True, vmem_limit_bytes=63 * 1024 * 1024),
    )(gains, shifts, tokens, *weights)


def post_norm(values, gain, shift):
    mean = jnp.mean(values, axis=-1, keepdims=True)
    spread = jnp.mean(jnp.square(values - mean), axis=-1, keepdims=True)
    normed = (values - mean) * lax.rsqrt(spread + 1e-05)
    return (normed * gain + shift).astype(jnp.bfloat16)


def rounded_term(stream_rows, down_full):
    return jnp.dot(stream_rows, down_full, preferred_element_type=jnp.float32).astype(jnp.bfloat16)


def half_step(stream, gate_w, up_w, down_w, gain, shift):
    width = gate_w.shape[1]
    joined = jnp.concatenate(
        (
            lax.all_gather(gate_w, "fs", axis=0, tiled=True),
            lax.all_gather(up_w, "fs", axis=0, tiled=True),
        ),
        axis=1,
    )
    both = jnp.dot(stream, joined, preferred_element_type=jnp.float32)
    gate = both[:, :width]
    up = both[:, width:]
    hidden = (jax.nn.silu(gate) * up).astype(jnp.bfloat16)
    scale = 2.0**0.25
    down_full = lax.all_gather(down_w, "fs", axis=1, tiled=True)
    partial_value = rounded_term(hidden, down_full)
    branch = lax.psum(partial_value, "tp").astype(jnp.float32).astype(jnp.bfloat16)
    return post_norm(
        scale * stream.astype(jnp.float32) + 0.5 * branch.astype(jnp.float32), gain, shift
    )


def local(
    tokens,
    norm_gain,
    norm_shift,
    gate_first,
    up_first,
    down_first,
    gate_second,
    up_second,
    down_second,
):
    middle = half_step(tokens, gate_first, up_first, down_first, norm_gain[0], norm_shift[0])
    return half_step(middle, gate_second, up_second, down_second, norm_gain[1], norm_shift[1])


def fits(mesh, args):
    tokens, gate_first = args[0], args[3]
    nf, nt = mesh.shape["fs"], mesh.shape["tp"]
    depth, units = gate_first.shape
    return (
        mesh.shape["grp"] == 2 and nt % 2 == 0 and nf == 4
        and depth % 128 == 0 and units % 128 == 0 and tokens.shape[0] % 64 == 0
    )


def solution(mesh):
    def either(*args):
        if fits(mesh, args):
            return fused(mesh.shape["fs"], mesh.shape["tp"], *args)
        return local(*args)

    placed = (
        P(("grp", "fs"), None),
        P(),
        P(),
        P("fs", "tp"),
        P("fs", "tp"),
        P("tp", "fs"),
        P("fs", "tp"),
        P("fs", "tp"),
        P("tp", "fs"),
    )
    return jax.shard_map(
        either, mesh=mesh, in_specs=placed, out_specs=P(("grp", "fs"), None), check_vma=False
    )
```

```python
import functools

import jax
import jax.numpy as jnp
from jax import lax
from jax.experimental import pallas as pl
from jax.experimental.pallas import tpu as pltpu
from jax.sharding import PartitionSpec as P

MESH = pl.DeviceIdType.MESH
SCALE = 2.0**0.25
F32 = jnp.float32
BF16 = jnp.bfloat16


def aligned(value, step):
    return pl.multiple_of(value, step)


def fused_kernel(nf, nt, *refs):
    gains, shifts, tokens = refs[:3]
    shards = refs[3:9]
    out = refs[9]
    full = refs[10:16]
    stream, gate, hidden, part, middle, pair, ring = refs[16:23]
    (z_recv, extra_recv, y_recv, line_sent, mate_sent, extra_sent, y_sent, own_done,
     core_sent, core_recv, x_sent, x_recv, back_sent, back_recv,
     swap_sent, swap_recv, hand_sent, hand_recv, tokens_done, spread_sent, spread_recv) = refs[23:]

    g = lax.axis_index("grp")
    f = lax.axis_index("fs")
    t = lax.axis_index("tp")
    other_g = 1 - g
    chip, core = t // 2, t % 2
    chips = nt // 2
    peer = chip * 2 + (1 - core)
    rows, width = tokens.shape
    half = rows // 2
    depth = width // nf

    at_end = (f == 0) | (f == nf - 1)
    inside = (f > 0) & (f < nf - 1)
    low = f < nf // 2
    mate = jnp.where(low, 1 - f, 2 * nf - 3 - f)
    facing = nf - 1 - f
    far = nf - 1 - mate
    mine = pl.ds(aligned(core * half, half), half)
    theirs = pl.ds(aligned((1 - core) * half, half), half)

    def tell(**where):
        pl.semaphore_signal(barrier, inc=1, device_id=where, device_id_type=MESH)

    barrier = pltpu.get_barrier_semaphore()
    tell(fs=mate)
    pl.when(inside)(lambda: tell(fs=facing))
    tell(grp=other_g)
    tell(tp=peer)
    for step in range(1, chips):
        tell(tp=lax.rem(chip + step, chips) * 2 + core)
    pl.semaphore_wait(barrier, jnp.where(inside, 1, 0) + 2 + chips)

    def remote(src, dst, sent, received, **where):
        return pltpu.make_async_remote_copy(
            src, dst, sent, received, device_id=where, device_id_type=MESH)

    def shard_part(a, which):
        size = shards[a].shape[0] // 2
        return shards[a].at[pl.ds(aligned(which * size, size), size), :]

    def slot(a, s, which):
        if a % 3 == 2:
            size = full[a].shape[1] // 2
            return full[a].at[s, pl.ds(aligned(which * size, size), size), :]
        size = depth // 2
        return full[a].at[pl.ds(aligned(s * depth + which * size, size), size), :]

    def whole_slot(a, s):
        if a % 3 == 2:
            return full[a].at[s]
        return full[a].at[pl.ds(aligned(s * depth, depth), depth), :]

    def columns(s):
        return pl.ds(aligned(s * depth, depth), depth)

    both_parts = range(6)

    def own(a):
        return pltpu.make_async_copy(shards[a], whole_slot(a, f), own_done.at[a])

    def from_end(a, s):
        return remote(shard_part(a, g), slot(a, s, g), mate_sent.at[a], z_recv.at[a, s], fs=mate)

    def extra(a, s):
        return remote(
            shard_part(a, other_g), slot(a, s, other_g), extra_sent.at[a], extra_recv.at[a],
            fs=mate)

    def along(a, s, src):
        return remote(src, slot(a, s, g), line_sent.at[a, s], z_recv.at[a, s], fs=facing)

    def across(a, s, which):
        return remote(
            slot(a, s, which), slot(a, s, which), y_sent.at[a, s], y_recv.at[a, s], grp=other_g)

    def hand_tokens():
        return remote(
            tokens.at[piece(chip), :], stream.at[1, piece(chip), :],
            hand_sent.at[0], hand_recv.at[0], fs=mate)

    def piece(which):
        size = half // chips
        return pl.ds(aligned(core * half + which * size, size), size)

    def spread_tokens(source, target):
        return remote(
            stream.at[1, piece(source), :], stream.at[1, piece(source), :],
            spread_sent.at[target], spread_recv.at[source], tp=target * 2 + core)

    def share_tokens(where):
        return remote(
            stream.at[1, where, :], stream.at[1, where, :], hand_sent.at[1], hand_recv.at[1],
            tp=peer)

    def hand_middle():
        return remote(
            middle.at[1, mine, :], middle.at[0, mine, :], hand_sent.at[2], hand_recv.at[2],
            fs=mate)

    def core_copy(layer, s):
        return remote(
            part.at[layer, :, theirs, columns(s)], pair.at[layer, :, :, columns(s)],
            core_sent.at[layer, s], core_recv.at[layer, s], tp=peer)

    def x_view(layer, s, source):
        if layer == 0:
            return ring.at[0, source, :, :, columns(s)]
        return ring.at[1, source, 0, :, columns(s)]

    def x_copy(layer, s, source, target):
        return remote(
            x_view(layer, s, source), x_view(layer, s, source),
            x_sent.at[layer, s, target], x_recv.at[layer, s, source], tp=target * 2 + core)

    def back(s):
        return remote(
            ring.at[1, chip, 1, :, columns(s)], ring.at[1, chip, 0, :, columns(s)],
            back_sent.at[s], back_recv.at[s], fs=mate)

    def swap(layer, where):
        view = middle.at[:, where, :] if layer == 0 else out.at[where, :]
        return remote(view, view, swap_sent.at[layer], swap_recv.at[layer], tp=peer)

    def x_start(layer, s):
        for step in range(1, chips):
            x_copy(layer, s, chip, lax.rem(chip + step, chips)).start()

    def x_arrived(layer, s):
        for step in range(1, chips):
            source = lax.rem(chip + step, chips)
            x_copy(layer, s, source, source).wait_recv()

    def x_left(layer, s):
        for step in range(1, chips):
            x_copy(layer, s, chip, lax.rem(chip + step, chips)).wait_send()

    tile = 256 if gate.shape[2] % 256 == 0 else gate.shape[2]
    tiles = gate.shape[2] // tile

    def project_gate(a, source):
        @pl.loop(0, 2 * tiles)
        def _(i):
            block, cols = i // tiles, pl.ds(aligned((i % tiles) * tile, tile), tile)
            gate[block, :, cols] = jnp.dot(
                source[block], full[a][:, cols], preferred_element_type=F32)

    def project_up(a, source):
        @pl.loop(0, 2 * tiles)
        def _(i):
            block, cols = i // tiles, pl.ds(aligned((i % tiles) * tile, tile), tile)
            up = jnp.dot(source[block], full[a][:, cols], preferred_element_type=F32)
            hidden[block, :, cols] = (jax.nn.silu(gate[block, :, cols]) * up).astype(BF16)

    def partial(layer, s):
        @pl.loop(0, 2)
        def _(block):
            part[layer, block, :, columns(s)] = jnp.dot(
                hidden[block], full[3 * layer + 2][s], preferred_element_type=F32).astype(BF16)
        core_copy(layer, s).start()

    def pair_sum(layer, s):
        core_copy(layer, s).wait_recv()
        for block in (1, 0):
            ring[layer, chip, block, :, columns(s)] = (
                part[layer, block, mine, columns(s)].astype(F32)
                + pair[layer, block, :, columns(s)].astype(F32)
            ).astype(BF16)
            if layer == 1 and block == 1:
                back(s).start()
        x_start(layer, s)

    def norm(layer, block, source, target):
        band = 32

        @pl.loop(0, half // band)
        def _(i):
            here = pl.ds(aligned(i * band, band), band)
            there = pl.ds(aligned(core * half + i * band, band), band)
            total = ring[layer, 0, block, here, :].astype(F32)
            for c in range(1, chips):
                total = total + ring[layer, c, block, here, :].astype(F32)
            branch = total.astype(BF16).astype(F32)
            v = SCALE * source[block, there, :].astype(F32) + 0.5 * branch
            v = v - jnp.mean(v, axis=-1, keepdims=True)
            spread = jnp.mean(v * v, axis=-1, keepdims=True)
            normed = v * lax.rsqrt(spread + 1e-05)
            done = (normed * gains[layer:layer + 1, :] + shifts[layer:layer + 1, :]).astype(BF16)
            if layer == 0:
                target[block, there, :] = done
            else:
                target[there, :] = done

    def finish():
        norm(1, 0, middle, out)
        swap(1, mine).start()
        swap(1, theirs).wait_recv()
        swap(1, mine).wait_send()

    @pl.when(at_end)
    def _():
        queue = [from_end(0, f), hand_tokens()]
        for a in range(1, 6):
            queue.append(from_end(a, f))
            if a - 1 in both_parts:
                queue.append(extra(a - 1, f))
        queue.append(extra(5, f))
        for k, copy in enumerate(queue):
            if k >= 2:
                queue[k - 2].wait_send()
            copy.start()
        queue[-2].wait_send()
        queue[-1].wait_send()
        hand_middle().wait_recv()
        for s in (mate, f, nf - 1 - mate, nf - 1 - f):
            back(s).wait_recv()
            x_start(1, s)
        pl.loop(0, nf)(lambda s: x_arrived(1, s))
        finish()
        pl.loop(0, nf)(lambda s: x_left(1, s))

    def mate_part(a):
        from_end(a, mate).wait_recv()
        along(a, mate, slot(a, mate, g)).start()
        if a not in both_parts:
            across(a, mate, g).start()

    def line_part(a, s):
        along(a, s, slot(a, s, g)).wait_recv()
        across(a, s, g).start()

    def mate_whole(a):
        if a in both_parts:
            extra(a, mate).wait_recv()
        else:
            across(a, mate, other_g).wait_recv()

    def crossed(a, s):
        across(a, s, other_g).wait_recv()

    def arrived(a):
        own(a).wait()
        mate_whole(a)
        crossed(a, facing)
        crossed(a, far)

    @pl.when(inside)
    def _():
        along(0, f, shard_part(0, g)).start()
        along(1, f, shard_part(1, g)).start()
        own_tokens = pltpu.make_async_copy(tokens, stream.at[0], tokens_done)
        own_tokens.start()
        for a in range(6):
            own(a).start()

        for a in range(6):
            if a < 4:
                along(a + 2, f, shard_part(a + 2, g)).start()
            if a == 0:
                line_part(a, facing)
                mate_part(a)
            else:
                mate_part(a)
                line_part(a, facing)
            if a == 1:
                others = [lax.rem(chip + step, chips) for step in range(1, chips)]
                hand_tokens().wait_recv()
                for c in others:
                    spread_tokens(chip, c).start()
                for c in others:
                    spread_tokens(c, c).wait_recv()
                share_tokens(mine).start()
                own_tokens.wait()
                share_tokens(theirs).wait_recv()
                arrived(0)
                project_gate(0, stream)
            if a == 2:
                arrived(1)
                project_up(1, stream)
                own(2).wait()
                partial(0, f)
                mate_whole(2)
                partial(0, mate)
                pair_sum(0, f)
            if a == 3:
                crossed(2, facing)
                partial(0, facing)
                pair_sum(0, mate)
            line_part(a, far)
            if a == 3:
                crossed(2, far)
                partial(0, far)
                pair_sum(0, facing)
                pair_sum(0, far)

        pl.loop(0, nf)(lambda s: x_arrived(0, s))
        norm(0, 0, stream, middle)
        norm(0, 1, stream, middle)
        swap(0, mine).start()
        hand_middle().start()
        swap(0, theirs).wait_recv()
        arrived(3)
        project_gate(3, middle)
        arrived(4)
        project_up(4, middle)
        own(5).wait()
        partial(1, f)
        mate_whole(5)
        partial(1, mate)
        pair_sum(1, f)
        crossed(5, facing)
        partial(1, facing)
        pair_sum(1, mate)
        crossed(5, far)
        partial(1, far)
        pair_sum(1, facing)
        pair_sum(1, far)
        pl.loop(0, nf)(lambda s: x_arrived(1, s))
        finish()

        share_tokens(mine).wait_send()
        for step in range(1, chips):
            spread_tokens(chip, lax.rem(chip + step, chips)).wait_send()
        hand_middle().wait_send()
        swap(0, mine).wait_send()
        for a in range(6):
            along(a, f, slot(a, f, g)).wait_send()
            along(a, mate, slot(a, mate, g)).wait_send()
            across(a, facing, g).wait_send()
            across(a, far, g).wait_send()
            if a not in both_parts:
                across(a, mate, g).wait_send()

        @pl.loop(0, nf)
        def _(s):
            back(s).wait_send()
            for layer in range(2):
                core_copy(layer, s).wait_send()
                x_left(layer, s)


def fused(nf, nt, tokens, gains, shifts, *weights):
    rows, width = tokens.shape
    units = weights[0].shape[1]
    depth = width // nf
    half = rows // 2
    side = pltpu.VMEM((width, units), BF16)
    down = pltpu.VMEM((nf, units, depth), BF16)
    dma = pltpu.SemaphoreType.DMA
    chips = nt // 2
    return pl.pallas_call(
        functools.partial(fused_kernel, nf, nt),
        out_shape=jax.ShapeDtypeStruct((rows, width), BF16),
        in_specs=[pl.BlockSpec(memory_space=pltpu.VMEM)] * 2
        + [pl.BlockSpec(memory_space=pl.ANY)] * 7,
        out_specs=pl.BlockSpec(memory_space=pltpu.VMEM),
        scratch_shapes=[
            side, side, down, side, side, down,
            pltpu.VMEM((2, rows, width), BF16),
            pltpu.VMEM((2, rows, units), F32),
            pltpu.VMEM((2, rows, units), BF16),
            pltpu.VMEM((2, 2, rows, width), BF16),
            pltpu.VMEM((2, rows, width), BF16),
            pltpu.VMEM((2, 2, half, width), BF16),
            pltpu.VMEM((2, chips, 2, half, width), BF16),
            dma((6, nf)), dma((6,)), dma((6, nf)), dma((6, nf)), dma((6,)), dma((6,)),
            dma((6, nf)), dma((6,)),
            dma((2, nf)), dma((2, nf)), dma((2, nf, chips)), dma((2, nf, chips)),
            dma((nf,)), dma((nf,)),
            dma((2,)), dma((2,)), dma((3,)), dma((3,)), dma,
            dma((chips,)), dma((chips,)),
        ],
        compiler_params=pltpu.CompilerParams(
            collective_id=0, has_side_effects=True, vmem_limit_bytes=63 * 1024 * 1024),
    )(gains, shifts, tokens, *weights)


def post_norm(values, gain, shift):
    mean = jnp.mean(values, axis=-1, keepdims=True)
    spread = jnp.mean(jnp.square(values - mean), axis=-1, keepdims=True)
    normed = (values - mean) * lax.rsqrt(spread + 1e-05)
    return (normed * gain + shift).astype(jnp.bfloat16)


def rounded_term(stream_rows, down_full):
    return jnp.dot(stream_rows, down_full, preferred_element_type=jnp.float32).astype(jnp.bfloat16)


def half_step(stream, gate_w, up_w, down_w, gain, shift):
    width = gate_w.shape[1]
    joined = jnp.concatenate(
        (
            lax.all_gather(gate_w, "fs", axis=0, tiled=True),
            lax.all_gather(up_w, "fs", axis=0, tiled=True),
        ),
        axis=1,
    )
    both = jnp.dot(stream, joined, preferred_element_type=jnp.float32)
    gate = both[:, :width]
    up = both[:, width:]
    hidden = (jax.nn.silu(gate) * up).astype(jnp.bfloat16)
    scale = 2.0**0.25
    down_full = lax.all_gather(down_w, "fs", axis=1, tiled=True)
    partial_value = rounded_term(hidden, down_full)
    branch = lax.psum(partial_value, "tp").astype(jnp.float32).astype(jnp.bfloat16)
    return post_norm(
        scale * stream.astype(jnp.float32) + 0.5 * branch.astype(jnp.float32), gain, shift
    )


def local(
    tokens,
    norm_gain,
    norm_shift,
    gate_first,
    up_first,
    down_first,
    gate_second,
    up_second,
    down_second,
):
    middle = half_step(tokens, gate_first, up_first, down_first, norm_gain[0], norm_shift[0])
    return half_step(middle, gate_second, up_second, down_second, norm_gain[1], norm_shift[1])


def fits(mesh, args):
    tokens, gate_first = args[0], args[3]
    nf, nt = mesh.shape["fs"], mesh.shape["tp"]
    depth, units = gate_first.shape
    return (
        mesh.shape["grp"] == 2 and nt % 2 == 0 and nf == 4
        and depth % 128 == 0 and units % 128 == 0 and tokens.shape[0] % 64 == 0
    )


def solution(mesh):
    def either(*args):
        if fits(mesh, args):
            return fused(mesh.shape["fs"], mesh.shape["tp"], *args)
        return local(*args)

    placed = (
        P(("grp", "fs"), None),
        P(),
        P(),
        P("fs", "tp"),
        P("fs", "tp"),
        P("tp", "fs"),
        P("fs", "tp"),
        P("fs", "tp"),
        P("tp", "fs"),
    )
    return jax.shard_map(
        either, mesh=mesh, in_specs=placed, out_specs=P(("grp", "fs"), None), check_vma=False
    )
```
